32 devices in a mesh: kv: 8 (over z, x), tp: 4 (over y, core).
Axes of the slice: x: 2, y: 2, z: 4, core: 2. Of those that a mesh axis runs over, the one named last changes fastest.
Arguments:
- stream: bfloat16 [128, 4096], P(None, ('kv', 'tp')), may hold values from -20 to 20
- ssm_state: float32 [128, 64, 64, 128], P('kv', 'tp'), may hold values from -1.8 to 1.8
- conv_state: bfloat16 [128, 3, 8, 768], P('kv', None, 'tp'), may hold values from -6 to 6
- first_gain: float32 [4096], P(('kv', 'tp')), may hold values from 0.1 to 1.9
- first_gate: bfloat16 [4096, 11264], P('kv', 'tp'), may hold values from -0.09375 to 0.09375
- first_up: bfloat16 [4096, 11264], P('kv', 'tp'), may hold values from -0.09375 to 0.09375
- first_down: bfloat16 [11264, 4096], P('tp', 'kv'), may hold values from -0.0546875 to 0.0546875
- mix_gain: float32 [4096], P(('kv', 'tp')), may hold values from 0.1 to 1.9
- gate_in: bfloat16 [4096, 4096], P('kv', 'tp'), may hold values from -0.09375 to 0.09375
- value_in: bfloat16 [4096, 4096], P('kv', 'tp'), may hold values from -0.09375 to 0.09375
- write_in: bfloat16 [4096, 1024], P('kv', 'tp'), may hold values from -0.09375 to 0.09375
- read_in: bfloat16 [4096, 1024], P('kv', 'tp'), may hold values from -0.09375 to 0.09375
- step_in: bfloat16 [4096, 64], P('kv', 'tp'), may hold values from -0.09375 to 0.09375
- conv_weight: float32 [4, 8, 768], P(None, 'tp'), may hold values from -3 to 3
- step_bias: float32 [64], P('tp'), may hold values from -3 to 0.5
- log_decay_rate: float32 [64], P('tp'), may hold values from -1 to 2.5
- group_gain: float32 [4096], P('tp'), may hold values from 0.1 to 1.9
- out_weight: bfloat16 [4096, 4096], P('tp', 'kv'), may hold values from -0.09375 to 0.09375
- last_norm_gain: float32 [4096], P(('kv', 'tp')), may hold values from 0.1 to 1.9
- second_gate: bfloat16 [4096, 11264], P('kv', 'tp'), may hold values from -0.09375 to 0.09375
- second_up: bfloat16 [4096, 11264], P('kv', 'tp'), may hold values from -0.09375 to 0.09375
- second_down: bfloat16 [11264, 4096], P('tp', 'kv'), may hold values from -0.109375 to 0.109375
Outputs:
- next_stream: bfloat16 [128, 4096], P(None, ('kv', 'tp'))
- ssm_next: float32 [128, 64, 64, 128], P('kv', 'tp')
- conv_next: bfloat16 [128, 3, 8, 768], P('kv', None, 'tp')
The draws below stay inside these ranges and needn't reach their ends.
All inputs are finite; a program needn't handle non-finite values.
Results may differ from the reference program's by a relative error of at most 0.015.
Values may be sent and summed in bfloat16 or wider, within the bound.
A program may use at most 128 MiB of HBM per device.

```python
import jax
import jax.numpy as jnp
from jax import lax

D = 4096
FF = 11264
HEADS = 64
HEAD_DIM = 64
STATE = 128
GROUPS = 8
TAPS = 4
SEQS = 128
GROUP_CH = 768
N_KV = 8
N_TP = 4


def draw_stream(key, part):
    noise_key = jax.random.fold_in(jax.random.fold_in(key, 11), 0)
    shard_width = D // (N_KV * N_TP)
    column = jnp.arange(D, dtype=jnp.int32)
    tp_index = column // shard_width % N_TP
    kv_index = column // (shard_width * N_TP)
    tp_frac = tp_index.astype(jnp.float32) / max(N_TP - 1, 1)
    kv_frac = kv_index.astype(jnp.float32) / max(N_KV - 1, 1)
    column_scale = jnp.exp(jnp.log(0.3) + jnp.log(10.0) * tp_frac + jnp.log(1.3) * kv_frac)[None]
    base = jax.random.truncated_normal(noise_key, -4.0, 4.0, (SEQS, D), jnp.float32)
    return (base * column_scale).astype(jnp.bfloat16)


def level_of(rng, dims, cuts, least, high):
    def one(dim, blocks):
        steps = jax.random.uniform(jax.random.fold_in(jax.random.fold_in(rng, 6), dim), (blocks,), jnp.float32, least / len(cuts), high / len(cuts))
        return jnp.repeat(jnp.exp(steps), dims[dim] // blocks).reshape((-1,) + (1,) * (len(dims) - dim - 1))

    loudness = one(*cuts[0])
    for cut in cuts[1:]:
        loudness = loudness * one(*cut)
    return loudness


def scatter_about(key, dims, scale, limit, pieces=(), held_as=jnp.bfloat16):
    result = scale * jax.random.normal(key, dims, jnp.float32)
    if pieces:
        result = result * level_of(key, dims, pieces, -0.22, 0.18)
    return jnp.clip(result, -limit, limit).astype(held_as)


def setup_inputs(seed: int = 0) -> dict:
    seeds = jax.random.split(jax.random.key(seed), 23)
    stream = draw_stream(jax.random.fold_in(seeds[22], 71), 0)
    ssm_state = scatter_about(seeds[1], (SEQS, HEADS, HEAD_DIM, STATE), 0.3, 1.8, ((0, 8), (1, 4)), jnp.float32)
    conv_state = scatter_about(seeds[2], (SEQS, TAPS - 1, GROUPS, GROUP_CH), 1.0, 6.0, ((0, 8), (2, 4)))
    first_gain = jnp.clip(1.0 + 0.18 * jax.random.normal(seeds[3], (D,), jnp.float32), 0.1, 1.9)
    first_gate = scatter_about(seeds[4], (D, FF), D ** -0.5, 0.09375, ((0, 8), (1, 4)))
    first_up = scatter_about(seeds[5], (D, FF), D ** -0.5, 0.09375, ((0, 8), (1, 4)))
    first_down = scatter_about(seeds[6], (FF, D), FF ** -0.5, 0.0546875, ((0, 4), (1, 8)))
    mix_gain = jnp.clip(1.0 + 0.18 * jax.random.normal(seeds[7], (D,), jnp.float32), 0.1, 1.9)
    gate_in = scatter_about(seeds[8], (D, HEADS * HEAD_DIM), D ** -0.5, 0.09375, ((0, 8), (1, 4)))
    value_in = scatter_about(seeds[9], (D, HEADS * HEAD_DIM), D ** -0.5, 0.09375, ((0, 8), (1, 4)))
    write_in = scatter_about(seeds[10], (D, GROUPS * STATE), D ** -0.5, 0.09375, ((0, 8), (1, 4)))
    read_in = scatter_about(seeds[11], (D, GROUPS * STATE), D ** -0.5, 0.09375, ((0, 8), (1, 4)))
    step_in = scatter_about(seeds[12], (D, HEADS), D ** -0.5, 0.09375, ((0, 8), (1, 4)))
    conv_weight = scatter_about(seeds[13], (TAPS, GROUPS, GROUP_CH), TAPS ** -0.5, 3.0, ((1, 4),), jnp.float32)
    step_bias = jnp.clip(-3.0 + 3.5 * jax.random.uniform(seeds[14], (HEADS,), jnp.float32) ** level_of(seeds[14], (HEADS,), ((0, 4),), -0.2, 0.2), -3.0, 0.5)
    log_decay_rate = jnp.clip(-1.0 + 3.5 * jax.random.uniform(seeds[15], (HEADS,), jnp.float32) ** level_of(seeds[15], (HEADS,), ((0, 4),), -0.2, 0.2), -1.0, 2.5)
    group_gain = jnp.clip(1.0 + 0.18 * jax.random.normal(seeds[16], (HEADS * HEAD_DIM,), jnp.float32), 0.1, 1.9)
    out_weight = scatter_about(seeds[17], (HEADS * HEAD_DIM, D), (HEADS * HEAD_DIM) ** -0.5, 0.09375, ((0, 4), (1, 8)))
    last_norm_gain = jnp.clip(1.0 + 0.18 * jax.random.normal(seeds[18], (D,), jnp.float32), 0.1, 1.9)
    second_gate = scatter_about(seeds[19], (D, FF), D ** -0.5, 0.09375, ((0, 8), (1, 4)))
    second_up = scatter_about(seeds[20], (D, FF), D ** -0.5, 0.09375, ((0, 8), (1, 4)))
    second_down = scatter_about(seeds[21], (FF, D), (FF // 4) ** -0.5, 0.109375, ((0, 4), (1, 8)))
    return dict(stream=stream, ssm_state=ssm_state, conv_state=conv_state, first_gain=first_gain, first_gate=first_gate, first_up=first_up, first_down=first_down, mix_gain=mix_gain, gate_in=gate_in, value_in=value_in, write_in=write_in, read_in=read_in, step_in=step_in, conv_weight=conv_weight, step_bias=step_bias, log_decay_rate=log_decay_rate, group_gain=group_gain, out_weight=out_weight, last_norm_gain=last_norm_gain, second_gate=second_gate, second_up=second_up, second_down=second_down)


norm_epsilon = 1e-06

def norm_rows(stream, gain):
    values = stream.astype(jnp.float32)
    scaled = (values * gain.astype(jnp.float32)[None]).astype(jnp.bfloat16)
    factor = lax.rsqrt(lax.optimization_barrier(jnp.mean(values * values, axis=1, keepdims=True)) + norm_epsilon)
    return (scaled, factor)

def blockwise_down(hidden, weight_matrix):
    batch = hidden.shape[0]
    block_list = hidden.reshape(batch, N_TP, -1).astype(jnp.float32)
    split_pieces = weight_matrix.reshape(N_TP, -1, weight_matrix.shape[1]).astype(jnp.float32)
    value_partial_sum = jnp.einsum('noc,oci->noi', block_list, split_pieces).astype(jnp.bfloat16)
    value_partial_sum = lax.optimization_barrier(value_partial_sum)
    return lax.optimization_barrier(jnp.sum(value_partial_sum.astype(jnp.float32), axis=1))

def channel_mixer(stream, gain, gate_weight, up_weight, down_weight):
    scaled, factor = norm_rows(stream, gain)
    gate = jnp.dot(scaled, gate_weight, preferred_element_type=jnp.float32) * factor
    up_sum = jnp.dot(scaled, up_weight, preferred_element_type=jnp.float32) * factor
    hidden = (jax.nn.silu(gate) * up_sum).astype(jnp.bfloat16)
    branch_output = blockwise_down(hidden, down_weight)
    return (stream.astype(jnp.float32) + 0.5 * branch_output).astype(jnp.bfloat16)

def token_mixer(stream, ssm_state, conv_state, gain, gate_in, value_in, write_in, read_in, step_in, conv_weight, step_bias, log_decay_rate, group_gain, out_weight):
    scaled, factor = norm_rows(stream, gain)

    def project(weight_matrix):
        return (jnp.dot(scaled, weight_matrix, preferred_element_type=jnp.float32) * factor).astype(jnp.bfloat16)
    gate = project(gate_in)
    values = project(value_in)
    writes = project(write_in)
    reads = project(read_in)
    steps = project(step_in)
    batch = stream.shape[0]
    groups = conv_weight.shape[1]
    state_size = write_in.shape[1] // groups
    heads = step_in.shape[1]
    head_size = value_in.shape[1] // heads
    per_group = heads // groups
    width = per_group * head_size
    fresh = jnp.concatenate([values.reshape(batch, groups, width), writes.reshape(batch, groups, state_size), reads.reshape(batch, groups, state_size)], axis=2)
    window = jnp.concatenate([conv_state, fresh[:, None]], axis=1)
    activated = jax.nn.silu(lax.optimization_barrier(jnp.sum(window.astype(jnp.float32) * conv_weight.astype(jnp.float32)[None], axis=1)))
    inputs = activated[:, :, :width].reshape(batch, groups, per_group, head_size)
    write_vec = activated[:, :, width:width + state_size]
    read_vec = activated[:, :, width + state_size:]
    step_size = jax.nn.softplus(steps.astype(jnp.float32) + step_bias[None])
    decay = jnp.exp(-step_size * jnp.exp(log_decay_rate)[None])
    step_size = step_size.reshape(batch, groups, per_group)
    decay = decay.reshape(batch, groups, per_group)
    carried = ssm_state.reshape(batch, groups, per_group, head_size, state_size)
    updated = carried * decay[:, :, :, None, None] + (step_size[:, :, :, None] * inputs)[..., None] * write_vec[:, :, None, None, :]
    readout = jnp.einsum('bghpn,bgn->bghp', updated, read_vec).reshape(batch, groups, width)
    gated = readout * jax.nn.silu(gate.astype(jnp.float32)).reshape(batch, groups, width)
    normed = gated * lax.rsqrt(lax.optimization_barrier(jnp.mean(gated * gated, axis=2, keepdims=True)) + norm_epsilon)
    mixed = (normed * group_gain.reshape(groups, width)[None]).astype(jnp.bfloat16).reshape(batch, groups * width)
    branch_output = blockwise_down(mixed, out_weight)
    after = (stream.astype(jnp.float32) + branch_output).astype(jnp.bfloat16)
    return (after, updated.reshape(ssm_state.shape), window[:, 1:])

def reference(stream, ssm_state, conv_state, first_gain, first_gate, first_up, first_down, mix_gain, gate_in, value_in, write_in, read_in, step_in, conv_weight, step_bias, log_decay_rate, group_gain, out_weight, last_norm_gain, second_gate, second_up, second_down):
    after_first = channel_mixer(stream, first_gain, first_gate, first_up, first_down)
    after_mix, ssm_next, conv_next = token_mixer(after_first, ssm_state, conv_state, mix_gain, gate_in, value_in, write_in, read_in, step_in, conv_weight, step_bias, log_decay_rate, group_gain, out_weight)
    next_stream = channel_mixer(after_mix, last_norm_gain, second_gate, second_up, second_down)
    return (next_stream, ssm_next, conv_next)
```

```python
import functools

import jax
import jax.numpy as jnp
from jax import lax
from jax.experimental import pallas as pl
from jax.experimental.pallas import tpu as pltpu
from jax.sharding import PartitionSpec as P

norm_epsilon = 1e-06
MESH = pl.DeviceIdType.MESH
LANES = 128
VM = pl.BlockSpec(memory_space=pltpu.VMEM)


def row_factor(total_squares, width):
    return lax.rsqrt(total_squares / width + norm_epsilon)[:, None]


def barrier(axis, n):
    me = lax.axis_index(axis)
    sem = pltpu.get_barrier_semaphore()
    for d in range(1, n):
        pl.semaphore_signal(sem, inc=1, device_id={axis: lax.rem(me + d, n)}, device_id_type=MESH)
    pl.semaphore_wait(sem, n - 1)


def remote(axis, peer, source, target, send, recv):
    return pltpu.make_async_remote_copy(
        src_ref=source,
        dst_ref=target,
        send_sem=send,
        recv_sem=recv,
        device_id={axis: peer},
        device_id_type=MESH,
    )


def block(ref, k, width, split):
    if split:
        return ref.at[k]
    return ref.at[:, pl.ds(pl.multiple_of(k * width, LANES), width)]


def scatter_start(axis, n, source_of, slots, send, recv):
    me = lax.axis_index(axis)
    copies = []
    for d in range(1, n):
        peer = lax.rem(me + d, n)
        copy = remote(axis, peer, source_of(peer), slots.at[d - 1], send.at[d - 1], recv.at[d - 1])
        copy.start()
        copies.append(copy)
    return copies


def gather(axis, n, target_of, send, recv):
    me = lax.axis_index(axis)
    copies = []
    for d in range(1, n):
        peer = lax.rem(me + d, n)
        copy = remote(axis, peer, target_of(me), target_of(me), send.at[d - 1], recv.at[d - 1])
        copy.start()
        copies.append(copy)
    for d in range(1, n):
        left = lax.rem(me - d + n, n)
        remote(axis, left, target_of(left), target_of(left), send.at[d - 1], recv.at[d - 1]).wait_recv()
    return copies


def call(kernel, outs, scratch, ident, *operands):
    return pl.pallas_call(
        kernel,
        out_shape=outs,
        in_specs=[VM] * len(operands),
        out_specs=jax.tree.map(lambda _: VM, outs),
        scratch_shapes=scratch,
        compiler_params=pltpu.CompilerParams(
            collective_id=ident, has_side_effects=True, vmem_limit_bytes=24 * 1024 * 1024
        ),
    )(*operands)


def sems(n):
    return pltpu.SemaphoreType.DMA((n - 1,))


def features_shape(rows, width, n, split):
    return (n, rows, width) if split else (rows, n * width)


def first_gather_kernel(n, split, stream_ref, gains_ref, out_ref, gains_out, s0, r0, s1, r1):
    width = stream_ref.shape[1]
    me = lax.axis_index("tp")
    if split:
        out_ref[me] = stream_ref[...]
    else:
        out_ref[:, pl.ds(pl.multiple_of(me * width, LANES), width)] = stream_ref[...]
    gains_out[me] = gains_ref[...]
    barrier("tp", n)
    copies = gather("tp", n, lambda k: block(out_ref, k, width, split), s0, r0)
    copies += gather("tp", n, lambda k: gains_out.at[k], s1, r1)
    for copy in copies:
        copy.wait_send()


def finish_kernel(n, split, weight, last, terms_ref, stream_ref, *refs):
    if last:
        after_ref, slots, s0, r0 = refs
    else:
        after_ref, out_ref, slots, s0, r0, s1, r1 = refs
    width = stream_ref.shape[1]
    me = lax.axis_index("tp")
    barrier("tp", n)
    copies = scatter_start("tp", n, lambda k: block(terms_ref, k, width, split), slots, s0, r0)
    if split:
        total = terms_ref[me].astype(jnp.float32)
    else:
        total = terms_ref[:, pl.ds(pl.multiple_of(me * width, LANES), width)].astype(jnp.float32)
    for d in range(1, n):
        copies[d - 1].wait_recv()
        total = total + slots[d - 1].astype(jnp.float32)
    after = (stream_ref[...].astype(jnp.float32) + weight * total).astype(jnp.bfloat16)
    after_ref[...] = after
    if not last:
        if split:
            out_ref[me] = after
        else:
            out_ref[:, pl.ds(pl.multiple_of(me * width, LANES), width)] = after
        copies += gather("tp", n, lambda k: block(out_ref, k, width, split), s1, r1)
    for copy in copies:
        copy.wait_send()


def hidden_kernel(n, width, gate_ref, up_ref, side_ref, out_ref, gate_in, up_in, side_in, sg, rg, su, ru, ss, rs, sh, rh):
    me = lax.axis_index("kv")
    barrier("kv", n)
    sides = scatter_start("kv", n, lambda k: side_ref.at[k], side_in, ss, rs)
    gates = scatter_start("kv", n, lambda k: gate_ref.at[k], gate_in, sg, rg)
    ups = scatter_start("kv", n, lambda k: up_ref.at[k], up_in, su, ru)
    for copy in sides + gates + ups:
        copy.wait_recv()
    squares = side_ref[me]
    for d in range(n - 1):
        squares = squares + side_in[d]
    factor = lax.rsqrt(squares / width + norm_epsilon)

    def tile(i, carry):
        cols = pl.ds(pl.multiple_of(i * LANES, LANES), LANES)
        gate = gate_ref[me, :, cols].astype(jnp.float32)
        up = up_ref[me, :, cols].astype(jnp.float32)
        for d in range(n - 1):
            gate = gate + gate_in[d, :, cols].astype(jnp.float32)
            up = up + up_in[d, :, cols].astype(jnp.float32)
        gate = gate * factor
        out_ref[me, :, cols] = (gate / (1.0 + jnp.exp(-gate)) * (up * factor)).astype(jnp.bfloat16)
        return carry

    lax.fori_loop(0, out_ref.shape[2] // LANES, tile, 0)
    copies = gather("kv", n, lambda k: out_ref.at[k], sh, rh)
    for copy in sides + gates + ups + copies:
        copy.wait_send()


def project_kernel(n, count, *refs):
    parts, outs, slots = refs[:count], refs[count : 2 * count], refs[2 * count : 3 * count]
    sem = refs[3 * count :]
    me = lax.axis_index("kv")
    barrier("kv", n)
    copies = []
    for i in range(count):
        copies.append(
            scatter_start("kv", n, lambda k, i=i: parts[i].at[k], slots[i], sem[2 * i], sem[2 * i + 1])
        )
    for i in range(count):
        for copy in copies[i]:
            copy.wait_recv()

        def tile(j, carry, i=i):
            cols = pl.ds(pl.multiple_of(j * LANES, LANES), LANES)
            total = parts[i][me, :, cols].astype(jnp.float32)
            for d in range(n - 1):
                total = total + slots[i][d, :, cols].astype(jnp.float32)
            outs[i][:, cols] = total
            return carry

        lax.fori_loop(0, outs[i].shape[1] // LANES, tile, 0)
    for group in copies:
        for copy in group:
            copy.wait_send()


def rows_gather_kernel(n, rows_ref, out_ref, s0, r0):
    out_ref[lax.axis_index("kv")] = rows_ref[...]
    barrier("kv", n)
    for copy in gather("kv", n, lambda k: out_ref.at[k], s0, r0):
        copy.wait_send()


def is_split(stream):
    return stream.shape[1] % LANES != 0


def joined(gathered, stream):
    if is_split(stream):
        return jnp.swapaxes(gathered, 0, 1).reshape(stream.shape[0], -1)
    return gathered


def normed_rows(features, gain):
    values = features.astype(jnp.float32)
    scaled = (values * gain[None]).astype(jnp.bfloat16)
    return (scaled, jnp.sum(values * values, axis=1))


def finish(stream, terms, weight, ident, last=False):
    n = lax.axis_size("tp")
    rows, width = stream.shape
    split = is_split(stream)
    terms = terms.astype(jnp.bfloat16)
    if split:
        terms = jnp.swapaxes(terms.reshape(rows, n, width), 0, 1)
    outs = [jax.ShapeDtypeStruct((rows, width), jnp.bfloat16)]
    scratch = [pltpu.VMEM((n - 1, rows, width), jnp.bfloat16), sems(n), sems(n)]
    if not last:
        outs.append(jax.ShapeDtypeStruct(features_shape(rows, width, n, split), jnp.bfloat16))
        scratch += [sems(n), sems(n)]
    result = call(
        functools.partial(finish_kernel, n, split, weight, last), outs, scratch, ident, terms, stream
    )
    if last:
        return result[0]
    return (result[0], joined(result[1], stream))


def hidden_units(features, gain, gate_weight, up_weight, ident):
    n = lax.axis_size("kv")
    rows, depth = features.shape
    count, units = rows // n, gate_weight.shape[1]
    scaled, squares = normed_rows(features, gain)
    gate = jnp.dot(scaled, gate_weight, preferred_element_type=jnp.float32).astype(jnp.bfloat16)
    up = jnp.dot(scaled, up_weight, preferred_element_type=jnp.float32).astype(jnp.bfloat16)
    side = jnp.broadcast_to(squares[:, None], (rows, LANES))
    hidden = call(
        functools.partial(hidden_kernel, n, depth * n),
        jax.ShapeDtypeStruct((n, count, units), jnp.bfloat16),
        [
            pltpu.VMEM((n - 1, count, units), jnp.bfloat16),
            pltpu.VMEM((n - 1, count, units), jnp.bfloat16),
            pltpu.VMEM((n - 1, count, LANES), jnp.float32),
        ]
        + [sems(n)] * 8,
        ident,
        gate.reshape(n, count, units),
        up.reshape(n, count, units),
        side.reshape(n, count, LANES),
    )
    return hidden.reshape(rows, units)


def projections(features, gain, gate_in, value_in, write_in, read_in, step_in, ident):
    n = lax.axis_size("kv")
    rows = features.shape[0]
    count = rows // n
    scaled, squares = normed_rows(features, gain)
    parts = [
        jnp.dot(scaled, w, preferred_element_type=jnp.float32).astype(jnp.bfloat16)
        for w in (gate_in, value_in, write_in, read_in)
    ]
    heads = step_in.shape[1]
    step = jnp.dot(scaled, step_in, preferred_element_type=jnp.float32)
    side_width = -(-(heads + 1) // LANES) * LANES
    parts.append(
        jnp.concatenate([step, jnp.broadcast_to(squares[:, None], (rows, side_width - heads))], axis=1)
    )
    parts = [p.reshape(n, count, p.shape[1]) for p in parts]
    sums = call(
        functools.partial(project_kernel, n, len(parts)),
        [jax.ShapeDtypeStruct(p.shape[1:], jnp.float32) for p in parts],
        [pltpu.VMEM((n - 1,) + p.shape[1:], p.dtype) for p in parts] + [sems(n)] * (2 * len(parts)),
        ident,
        *parts,
    )
    return (*sums[:4], sums[4][:, :heads], sums[4][:, heads])


def rows_gather(mixed, ident):
    n = lax.axis_size("kv")
    out = call(
        functools.partial(rows_gather_kernel, n),
        jax.ShapeDtypeStruct((n,) + mixed.shape, mixed.dtype),
        [sems(n), sems(n)],
        ident,
        mixed,
    )
    return out.reshape(n * mixed.shape[0], mixed.shape[1])


def first_gather(stream, gains):
    n = lax.axis_size("tp")
    rows, width = stream.shape
    split = is_split(stream)
    packed = jnp.stack(gains)
    out, packed = call(
        functools.partial(first_gather_kernel, n, split),
        [
            jax.ShapeDtypeStruct(features_shape(rows, width, n, split), stream.dtype),
            jax.ShapeDtypeStruct((n,) + packed.shape, packed.dtype),
        ],
        [sems(n)] * 4,
        0,
        stream,
        packed,
    )
    all_gains = jnp.swapaxes(packed, 0, 1).reshape(len(gains), n * width)
    return (joined(out, stream), all_gains)


def token_mixer(
    features,
    ssm_state,
    conv_state,
    gain,
    gate_in,
    value_in,
    write_in,
    read_in,
    step_in,
    conv_weight,
    step_bias,
    log_decay_rate,
    group_gain,
    out_weight,
):
    width_all = features.shape[1] * lax.axis_size("kv")
    count = features.shape[0] // lax.axis_size("kv")
    gate_sum, value_sum, write_sum, read_sum, step_sum, total = projections(
        features, gain, gate_in, value_in, write_in, read_in, step_in, 3
    )
    factor = row_factor(total, width_all)
    gate = (gate_sum * factor).astype(jnp.bfloat16)
    values = (value_sum * factor).astype(jnp.bfloat16)
    writes = (write_sum * factor).astype(jnp.bfloat16)
    reads = (read_sum * factor).astype(jnp.bfloat16)
    steps = (step_sum * factor).astype(jnp.bfloat16)
    groups = conv_weight.shape[1]
    state_size = write_in.shape[1] // groups
    heads = step_in.shape[1]
    head_size = value_in.shape[1] // heads
    per_group = heads // groups
    width = per_group * head_size
    fresh = jnp.concatenate(
        [
            values.reshape(count, groups, width),
            writes.reshape(count, groups, state_size),
            reads.reshape(count, groups, state_size),
        ],
        axis=2,
    )
    window = jnp.concatenate([conv_state, fresh[:, None]], axis=1)
    activated = jax.nn.silu(jnp.sum(window.astype(jnp.float32) * conv_weight[None], axis=1))
    inputs = activated[:, :, :width].reshape(count, groups, per_group, head_size)
    write_vec = activated[:, :, width : width + state_size]
    read_vec = activated[:, :, width + state_size :]
    step_size = jax.nn.softplus(steps.astype(jnp.float32) + step_bias[None])
    decay = jnp.exp(-step_size * jnp.exp(log_decay_rate)[None])
    step_size = step_size.reshape(count, groups, per_group)
    decay = decay.reshape(count, groups, per_group)
    carried = ssm_state.reshape(count, groups, per_group, head_size, state_size)
    updated = (
        carried * decay[:, :, :, None, None]
        + (step_size[:, :, :, None] * inputs)[..., None] * write_vec[:, :, None, None, :]
    )
    readout = jnp.einsum("bghpn,bgn->bghp", updated, read_vec).reshape(count, groups, width)
    gated = readout * jax.nn.silu(gate.astype(jnp.float32)).reshape(count, groups, width)
    normed = gated * lax.rsqrt(jnp.mean(gated * gated, axis=2, keepdims=True) + norm_epsilon)
    mixed = (
        (normed * group_gain.reshape(groups, width)[None])
        .astype(jnp.bfloat16)
        .reshape(count, groups * width)
    )
    terms = jnp.dot(rows_gather(mixed, 4), out_weight, preferred_element_type=jnp.float32)
    return (terms, updated.reshape(ssm_state.shape), window[:, 1:])


def on_device(
    stream,
    ssm_state,
    conv_state,
    first_gain,
    first_gate,
    first_up,
    first_down,
    mix_gain,
    gate_in,
    value_in,
    write_in,
    read_in,
    step_in,
    conv_weight,
    step_bias,
    log_decay_rate,
    group_gain,
    out_weight,
    last_norm_gain,
    second_gate,
    second_up,
    second_down,
):
    features, gains = first_gather(stream, [first_gain, mix_gain, last_norm_gain])
    hidden = hidden_units(features, gains[0], first_gate, first_up, 1)
    terms = jnp.dot(hidden, first_down, preferred_element_type=jnp.float32)
    after_first, features = finish(stream, terms, 0.5, 2)
    terms, ssm_next, conv_next = token_mixer(
        features,
        ssm_state,
        conv_state,
        gains[1],
        gate_in,
        value_in,
        write_in,
        read_in,
        step_in,
        conv_weight,
        step_bias,
        log_decay_rate,
        group_gain,
        out_weight,
    )
    after_mix, features = finish(after_first, terms, 1.0, 5)
    hidden = hidden_units(features, gains[2], second_gate, second_up, 6)
    terms = jnp.dot(hidden, second_down, preferred_element_type=jnp.float32)
    next_stream = finish(after_mix, terms, 0.5, 7, last=True)
    return (next_stream, ssm_next, conv_next)


def solution(mesh):
    return jax.shard_map(
        on_device,
        mesh=mesh,
        in_specs=(
            P(None, ("kv", "tp")),
            P("kv", "tp", None, None),
            P("kv", None, "tp", None),
            P(("kv", "tp")),
            P("kv", "tp"),
            P("kv", "tp"),
            P("tp", "kv"),
            P(("kv", "tp")),
            P("kv", "tp"),
            P("kv", "tp"),
            P("kv", "tp"),
            P("kv", "tp"),
            P("kv", "tp"),
            P(None, "tp", None),
            P("tp"),
            P("tp"),
            P("tp"),
            P("tp", "kv"),
            P(("kv", "tp")),
            P("kv", "tp"),
            P("kv", "tp"),
            P("tp", "kv"),
        ),
        out_specs=(P(None, ("kv", "tp")), P("kv", "tp", None, None), P("kv", None, "tp", None)),
        check_vma=False,
    )
```

```python
import functools

import jax
import jax.numpy as jnp
from jax import lax
from jax.experimental import pallas as pl
from jax.experimental.pallas import tpu as pltpu
from jax.sharding import PartitionSpec as P

norm_epsilon = 1e-06
MESH = pl.DeviceIdType.MESH
LANES = 128
VM = pl.BlockSpec(memory_space=pltpu.VMEM)


def row_factor(total_squares, width):
    return lax.rsqrt(total_squares / width + norm_epsilon)[:, None]


def barrier(axis, n):
    me = lax.axis_index(axis)
    sem = pltpu.get_barrier_semaphore()
    for d in range(1, n):
        pl.semaphore_signal(sem, inc=1, device_id={axis: lax.rem(me + d, n)}, device_id_type=MESH)
    pl.semaphore_wait(sem, n - 1)


def remote(axis, peer, source, target, send, recv):
    return pltpu.make_async_remote_copy(
        src_ref=source,
        dst_ref=target,
        send_sem=send,
        recv_sem=recv,
        device_id={axis: peer},
        device_id_type=MESH,
    )


def block(ref, k, width, split):
    if split:
        return ref.at[k]
    return ref.at[:, pl.ds(pl.multiple_of(k * width, LANES), width)]


def scatter_start(axis, n, source_of, slots, send, recv):
    me = lax.axis_index(axis)
    copies = []
    for d in range(1, n):
        peer = lax.rem(me + d, n)
        copy = remote(axis, peer, source_of(peer), slots.at[d - 1], send.at[d - 1], recv.at[d - 1])
        copy.start()
        copies.append(copy)
    return copies


def gather(axis, n, target_of, send, recv):
    me = lax.axis_index(axis)
    copies = []
    for d in range(1, n):
        peer = lax.rem(me + d, n)
        copy = remote(axis, peer, target_of(me), target_of(me), send.at[d - 1], recv.at[d - 1])
        copy.start()
        copies.append(copy)
    for d in range(1, n):
        left = lax.rem(me - d + n, n)
        remote(axis, left, target_of(left), target_of(left), send.at[d - 1], recv.at[d - 1]).wait_recv()
    return copies


def call(kernel, outs, scratch, ident, *operands):
    return pl.pallas_call(
        kernel,
        out_shape=outs,
        in_specs=[VM] * len(operands),
        out_specs=jax.tree.map(lambda _: VM, outs),
        scratch_shapes=scratch,
        compiler_params=pltpu.CompilerParams(
            collective_id=ident, has_side_effects=True, vmem_limit_bytes=24 * 1024 * 1024
        ),
    )(*operands)


def sems(n):
    return pltpu.SemaphoreType.DMA((n - 1,))


def features_shape(rows, width, n, split):
    return (n, rows, width) if split else (rows, n * width)


def first_gather_kernel(n, split, stream_ref, gains_ref, out_ref, gains_out, s0, r0, s1, r1):
    width = stream_ref.shape[1]
    me = lax.axis_index("tp")
    if split:
        out_ref[me] = stream_ref[...]
    else:
        out_ref[:, pl.ds(pl.multiple_of(me * width, LANES), width)] = stream_ref[...]
    gains_out[me] = gains_ref[...]
    barrier("tp", n)
    copies = gather("tp", n, lambda k: block(out_ref, k, width, split), s0, r0)
    copies += gather("tp", n, lambda k: gains_out.at[k], s1, r1)
    for copy in copies:
        copy.wait_send()


def finish_kernel(n, split, weight, last, terms_ref, stream_ref, *refs):
    if last:
        after_ref, slots, s0, r0 = refs
    else:
        after_ref, out_ref, slots, s0, r0, s1, r1 = refs
    width = stream_ref.shape[1]
    me = lax.axis_index("tp")
    barrier("tp", n)
    copies = scatter_start("tp", n, lambda k: block(terms_ref, k, width, split), slots, s0, r0)
    if split:
        total = terms_ref[me].astype(jnp.float32)
    else:
        total = terms_ref[:, pl.ds(pl.multiple_of(me * width, LANES), width)].astype(jnp.float32)
    for d in range(1, n):
        copies[d - 1].wait_recv()
        total = total + slots[d - 1].astype(jnp.float32)
    after = (stream_ref[...].astype(jnp.float32) + weight * total).astype(jnp.bfloat16)
    after_ref[...] = after
    if not last:
        if split:
            out_ref[me] = after
        else:
            out_ref[:, pl.ds(pl.multiple_of(me * width, LANES), width)] = after
        copies += gather("tp", n, lambda k: block(out_ref, k, width, split), s1, r1)
    for copy in copies:
        copy.wait_send()


def hidden_kernel(n, width, gate_ref, up_ref, side_ref, out_ref, side_in, *refs):
    zn, units = gate_ref.shape[0], gate_ref.shape[3]
    near, sums, far = refs[0:2], refs[2:4], refs[4:6]
    ss, rs, sa, ra, sz, rz, sh, rh, sx, rx = refs[6:]
    parts = (gate_ref, up_ref)
    me = lax.axis_index("kv")
    z, x = me // 2, lax.rem(me, 2)
    other = z * 2 + 1 - x
    tiles = units // LANES
    cuts = [tiles * i // 4 * LANES for i in range(5)]
    ranges = [pl.ds(lo, hi - lo) for lo, hi in zip(cuts, cuts[1:])]
    barrier("kv", n)
    sides = scatter_start("kv", n, lambda k: side_ref.at[k // 2, lax.rem(k, 2)], side_in, ss, rs)
    sent = list(sides)
    first = {}
    for c, cols in enumerate(ranges):
        for i in range(2):
            copy = remote(
                "kv", other, parts[i].at[:, 1 - x, :, cols], near[i].at[:, :, cols], sa.at[c, i], ra.at[c, i]
            )
            copy.start()
            first[c, i] = copy
            sent.append(copy)
    second = {}
    for c, cols in enumerate(ranges):
        for i in range(2):
            first[c, i].wait_recv()
            total = parts[i][:, x, :, cols].astype(jnp.float32) + near[i][:, :, cols].astype(jnp.float32)
            sums[i][:, :, cols] = total.astype(jnp.bfloat16)
            for d in range(1, zn):
                zp = lax.rem(z + d, zn)
                copy = remote(
                    "kv", zp * 2 + x, sums[i].at[zp, :, cols], far[i].at[d - 1, :, cols],
                    sz.at[c, i, d - 1], rz.at[c, i, d - 1],
                )
                copy.start()
                second[c, i, d] = copy
                sent.append(copy)
    for copy in sides:
        copy.wait_recv()
    squares = side_ref[z, x]
    for d in range(n - 1):
        squares = squares + side_in[d]
    factor = lax.rsqrt(squares / width + norm_epsilon)[:, :1]

    def spread(c, d, zq, xq, peer, send, recv):
        place = out_ref.at[zq, xq, :, ranges[c]]
        return remote("kv", peer, place, place, send.at[c, d], recv.at[c, d])

    for c, cols in enumerate(ranges):
        both = []
        for i in range(2):
            total = sums[i][z, :, cols].astype(jnp.float32)
            for d in range(1, zn):
                second[c, i, d].wait_recv()
                total = total + far[i][d - 1, :, cols].astype(jnp.float32)
            both.append(total * factor)
        gate, up = both
        out_ref[z, x, :, cols] = (gate / (1.0 + jnp.exp(-gate)) * up).astype(jnp.bfloat16)
        for d in range(1, zn):
            copy = spread(c, d - 1, z, x, lax.rem(z + d, zn) * 2 + x, sh, rh)
            copy.start()
            sent.append(copy)
        copy = spread(c, 0, z, x, other, sx, rx)
        copy.start()
        sent.append(copy)
    for c in range(4):
        for d in range(1, zn):
            left = lax.rem(z - d + zn, zn)
            spread(c, d - 1, left, x, left * 2 + x, sh, rh).wait_recv()
            copy = spread(c, d, left, x, other, sx, rx)
            copy.start()
            sent.append(copy)
    for c in range(4):
        for d in range(zn):
            left = lax.rem(z - d + zn, zn)
            spread(c, d, left, 1 - x, other, sx, rx).wait_recv()
    for copy in sent:
        copy.wait_send()


def project_kernel(n, count, *refs):
    parts, outs, slots = refs[:count], refs[count : 2 * count], refs[2 * count : 3 * count]
    sem = refs[3 * count :]
    me = lax.axis_index("kv")
    barrier("kv", n)
    copies = []
    for i in range(count):
        copies.append(
            scatter_start("kv", n, lambda k, i=i: parts[i].at[k], slots[i], sem[2 * i], sem[2 * i + 1])
        )
    for i in range(count):
        for copy in copies[i]:
            copy.wait_recv()

        def tile(j, carry, i=i):
            cols = pl.ds(pl.multiple_of(j * LANES, LANES), LANES)
            total = parts[i][me, :, cols].astype(jnp.float32)
            for d in range(n - 1):
                total = total + slots[i][d, :, cols].astype(jnp.float32)
            outs[i][:, cols] = total
            return carry

        lax.fori_loop(0, outs[i].shape[1] // LANES, tile, 0)
    for group in copies:
        for copy in group:
            copy.wait_send()


def rows_gather_kernel(n, rows_ref, out_ref, s0, r0):
    out_ref[lax.axis_index("kv")] = rows_ref[...]
    barrier("kv", n)
    for copy in gather("kv", n, lambda k: out_ref.at[k], s0, r0):
        copy.wait_send()


def is_split(stream):
    return stream.shape[1] % LANES != 0


def joined(gathered, stream):
    if is_split(stream):
        return jnp.swapaxes(gathered, 0, 1).reshape(stream.shape[0], -1)
    return gathered


def normed_rows(features, gain):
    values = features.astype(jnp.float32)
    scaled = (values * gain[None]).astype(jnp.bfloat16)
    return (scaled, jnp.sum(values * values, axis=1))


def finish(stream, terms, weight, ident, last=False):
    n = lax.axis_size("tp")
    rows, width = stream.shape
    split = is_split(stream)
    terms = terms.astype(jnp.bfloat16)
    if split:
        terms = jnp.swapaxes(terms.reshape(rows, n, width), 0, 1)
    outs = [jax.ShapeDtypeStruct((rows, width), jnp.bfloat16)]
    scratch = [pltpu.VMEM((n - 1, rows, width), jnp.bfloat16), sems(n), sems(n)]
    if not last:
        outs.append(jax.ShapeDtypeStruct(features_shape(rows, width, n, split), jnp.bfloat16))
        scratch += [sems(n), sems(n)]
    result = call(
        functools.partial(finish_kernel, n, split, weight, last), outs, scratch, ident, terms, stream
    )
    if last:
        return result[0]
    return (result[0], joined(result[1], stream))


def hidden_units(features, gain, gate_weight, up_weight, ident):
    n = lax.axis_size("kv")
    rows, depth = features.shape
    count, units = rows // n, gate_weight.shape[1]
    scaled, squares = normed_rows(features, gain)
    gate = jnp.dot(scaled, gate_weight, preferred_element_type=jnp.float32).astype(jnp.bfloat16)
    up = jnp.dot(scaled, up_weight, preferred_element_type=jnp.float32).astype(jnp.bfloat16)
    side = jnp.broadcast_to(squares[:, None], (rows, LANES))
    zn = n // 2
    dma = pltpu.SemaphoreType.DMA
    hidden = call(
        functools.partial(hidden_kernel, n, depth * n),
        jax.ShapeDtypeStruct((zn, 2, count, units), jnp.bfloat16),
        [pltpu.VMEM((n - 1, count, LANES), jnp.float32)]
        + [pltpu.VMEM((zn, count, units), jnp.bfloat16)] * 4
        + [pltpu.VMEM((zn - 1, count, units), jnp.bfloat16)] * 2
        + [sems(n)] * 2
        + [dma((4, 2))] * 2
        + [dma((4, 2, zn - 1))] * 2
        + [dma((4, zn - 1))] * 2
        + [dma((4, zn))] * 2,
        ident,
        gate.reshape(zn, 2, count, units),
        up.reshape(zn, 2, count, units),
        side.reshape(zn, 2, count, LANES),
    )
    return hidden.reshape(rows, units)


def projections(features, gain, gate_in, value_in, write_in, read_in, step_in, ident):
    n = lax.axis_size("kv")
    rows = features.shape[0]
    count = rows // n
    scaled, squares = normed_rows(features, gain)
    parts = [
        jnp.dot(scaled, w, preferred_element_type=jnp.float32).astype(jnp.bfloat16)
        for w in (gate_in, value_in, write_in, read_in)
    ]
    heads = step_in.shape[1]
    step = jnp.dot(scaled, step_in, preferred_element_type=jnp.float32)
    side_width = -(-(heads + 1) // LANES) * LANES
    parts.append(
        jnp.concatenate([step, jnp.broadcast_to(squares[:, None], (rows, side_width - heads))], axis=1)
    )
    parts = [p.reshape(n, count, p.shape[1]) for p in parts]
    sums = call(
        functools.partial(project_kernel, n, len(parts)),
        [jax.ShapeDtypeStruct(p.shape[1:], jnp.float32) for p in parts],
        [pltpu.VMEM((n - 1,) + p.shape[1:], p.dtype) for p in parts] + [sems(n)] * (2 * len(parts)),
        ident,
        *parts,
    )
    return (*sums[:4], sums[4][:, :heads], sums[4][:, heads])


def rows_gather(mixed, ident):
    n = lax.axis_size("kv")
    out = call(
        functools.partial(rows_gather_kernel, n),
        jax.ShapeDtypeStruct((n,) + mixed.shape, mixed.dtype),
        [sems(n), sems(n)],
        ident,
        mixed,
    )
    return out.reshape(n * mixed.shape[0], mixed.shape[1])


def first_gather(stream, gains):
    n = lax.axis_size("tp")
    rows, width = stream.shape
    split = is_split(stream)
    packed = jnp.stack(gains)
    out, packed = call(
        functools.partial(first_gather_kernel, n, split),
        [
            jax.ShapeDtypeStruct(features_shape(rows, width, n, split), stream.dtype),
            jax.ShapeDtypeStruct((n,) + packed.shape, packed.dtype),
        ],
        [sems(n)] * 4,
        0,
        stream,
        packed,
    )
    all_gains = jnp.swapaxes(packed, 0, 1).reshape(len(gains), n * width)
    return (joined(out, stream), all_gains)


def token_mixer(
    features,
    ssm_state,
    conv_state,
    gain,
    gate_in,
    value_in,
    write_in,
    read_in,
    step_in,
    conv_weight,
    step_bias,
    log_decay_rate,
    group_gain,
    out_weight,
):
    width_all = features.shape[1] * lax.axis_size("kv")
    count = features.shape[0] // lax.axis_size("kv")
    gate_sum, value_sum, write_sum, read_sum, step_sum, total = projections(
        features, gain, gate_in, value_in, write_in, read_in, step_in, 3
    )
    factor = row_factor(total, width_all)
    gate = (gate_sum * factor).astype(jnp.bfloat16)
    values = (value_sum * factor).astype(jnp.bfloat16)
    writes = (write_sum * factor).astype(jnp.bfloat16)
    reads = (read_sum * factor).astype(jnp.bfloat16)
    steps = (step_sum * factor).astype(jnp.bfloat16)
    groups = conv_weight.shape[1]
    state_size = write_in.shape[1] // groups
    heads = step_in.shape[1]
    head_size = value_in.shape[1] // heads
    per_group = heads // groups
    width = per_group * head_size
    fresh = jnp.concatenate(
        [
            values.reshape(count, groups, width),
            writes.reshape(count, groups, state_size),
            reads.reshape(count, groups, state_size),
        ],
        axis=2,
    )
    window = jnp.concatenate([conv_state, fresh[:, None]], axis=1)
    activated = jax.nn.silu(jnp.sum(window.astype(jnp.float32) * conv_weight[None], axis=1))
    inputs = activated[:, :, :width].reshape(count, groups, per_group, head_size)
    write_vec = activated[:, :, width : width + state_size]
    read_vec = activated[:, :, width + state_size :]
    step_size = jax.nn.softplus(steps.astype(jnp.float32) + step_bias[None])
    decay = jnp.exp(-step_size * jnp.exp(log_decay_rate)[None])
    step_size = step_size.reshape(count, groups, per_group)
    decay = decay.reshape(count, groups, per_group)
    carried = ssm_state.reshape(count, groups, per_group, head_size, state_size)
    updated = (
        carried * decay[:, :, :, None, None]
        + (step_size[:, :, :, None] * inputs)[..., None] * write_vec[:, :, None, None, :]
    )
    readout = jnp.einsum("bghpn,bgn->bghp", updated, read_vec).reshape(count, groups, width)
    gated = readout * jax.nn.silu(gate.astype(jnp.float32)).reshape(count, groups, width)
    normed = gated * lax.rsqrt(jnp.mean(gated * gated, axis=2, keepdims=True) + norm_epsilon)
    mixed = (
        (normed * group_gain.reshape(groups, width)[None])
        .astype(jnp.bfloat16)
        .reshape(count, groups * width)
    )
    terms = jnp.dot(rows_gather(mixed, 4), out_weight, preferred_element_type=jnp.float32)
    return (terms, updated.reshape(ssm_state.shape), window[:, 1:])


def on_device(
    stream,
    ssm_state,
    conv_state,
    first_gain,
    first_gate,
    first_up,
    first_down,
    mix_gain,
    gate_in,
    value_in,
    write_in,
    read_in,
    step_in,
    conv_weight,
    step_bias,
    log_decay_rate,
    group_gain,
    out_weight,
    last_norm_gain,
    second_gate,
    second_up,
    second_down,
):
    features, gains = first_gather(stream, [first_gain, mix_gain, last_norm_gain])
    hidden = hidden_units(features, gains[0], first_gate, first_up, 1)
    terms = jnp.dot(hidden, first_down, preferred_element_type=jnp.float32)
    after_first, features = finish(stream, terms, 0.5, 2)
    terms, ssm_next, conv_next = token_mixer(
        features,
        ssm_state,
        conv_state,
        gains[1],
        gate_in,
        value_in,
        write_in,
        read_in,
        step_in,
        conv_weight,
        step_bias,
        log_decay_rate,
        group_gain,
        out_weight,
    )
    after_mix, features = finish(after_first, terms, 1.0, 5)
    hidden = hidden_units(features, gains[2], second_gate, second_up, 6)
    terms = jnp.dot(hidden, second_down, preferred_element_type=jnp.float32)
    next_stream = finish(after_mix, terms, 0.5, 7, last=True)
    return (next_stream, ssm_next, conv_next)


def solution(mesh):
    return jax.shard_map(
        on_device,
        mesh=mesh,
        in_specs=(
            P(None, ("kv", "tp")),
            P("kv", "tp", None, None),
            P("kv", None, "tp", None),
            P(("kv", "tp")),
            P("kv", "tp"),
            P("kv", "tp"),
            P("tp", "kv"),
            P(("kv", "tp")),
            P("kv", "tp"),
            P("kv", "tp"),
            P("kv", "tp"),
            P("kv", "tp"),
            P("kv", "tp"),
            P(None, "tp", None),
            P("tp"),
            P("tp"),
            P("tp"),
            P("tp", "kv"),
            P(("kv", "tp")),
            P("kv", "tp"),
            P("kv", "tp"),
            P("tp", "kv"),
        ),
        out_specs=(P(None, ("kv", "tp")), P("kv", "tp", None, None), P("kv", None, "tp", None)),
        check_vma=False,
    )
```
